32 devices in a mesh: sp: 8 (over z, y), tp: 4 (over x, core).
Axes of the slice: x: 2, y: 2, z: 4, core: 2. Of those that a mesh axis runs over, the one named last changes fastest.
Arguments:
- hidden: bfloat16 [16, 512, 1024], P(None, 'sp'), may hold values from -0.09375 to 0.09375
- value_weight: bfloat16 [1024, 1024], P(None, 'tp'), may hold values from -0.75 to 0.75
- queries: bfloat16 [16, 8, 512, 64], P(None, 'tp', 'sp'), may hold values from -0.1875 to 0.1875
- key_vectors: bfloat16 [16, 8, 512, 64], P(None, 'tp', 'sp'), may hold values from -0.1875 to 0.1875
- forward_decay: float32 [16, 8, 512, 64], P(None, 'tp', 'sp'), may hold values from -0.005859375 to -1.953125e-05
- backward_decay: float32 [16, 8, 512, 64], P(None, 'tp', 'sp'), may hold values from -0.005859375 to -1.953125e-05
- cotangent: bfloat16 [16, 512, 1024], P(None, 'sp', 'tp'), may hold values from -6 to 6
Outputs:
- grad_queries: bfloat16 [16, 8, 512, 64], P(None, 'tp', 'sp')
- grad_keys: bfloat16 [16, 8, 512, 64], P(None, 'tp', 'sp')
- grad_forward: float32 [16, 8, 512, 64], P(None, 'tp', 'sp')
- grad_backward: float32 [16, 8, 512, 64], P(None, 'tp', 'sp')
- grad_hidden: bfloat16 [16, 512, 1024], P(None, 'sp', 'tp')
- grad_weight: float32 [1024, 1024], P('sp', 'tp')
The draws below stay inside these ranges and needn't reach their ends.
All inputs are finite; a program needn't handle non-finite values.
Results may differ from the reference program's by a relative error of at most 0.015.
Values may be sent and summed in bfloat16 or wider, within the bound.
A program may use at most 128 MiB of HBM per device.

```python
import jax
import jax.numpy as jnp
from jax import lax

D = 1024
HEADS = 8
DK = 64
DV = 128
BATCH = 16
TOK_DEV = 64
TOKENS = 512


def steps_of(rng, shape, cuts, smallest, high):
    level, own = 1.0, jax.random.fold_in(rng, 6)
    for axis_at, parts in cuts:
        heights = jnp.exp(jax.random.uniform(jax.random.fold_in(own, axis_at), (parts,), jnp.float32, smallest / len(cuts), high / len(cuts)))
        level = level * jnp.repeat(heights, shape[axis_at] // parts).reshape([-1 if axis == axis_at else 1 for axis in range(len(shape))])
    return level


def normal_values(key, dims, spread, reach, split=(), kind=jnp.bfloat16):
    values = jax.random.normal(key, dims, jnp.float32) * spread
    if len(split) > 0:
        values = steps_of(key, dims, split, -0.22, 0.18) * values
    return jnp.clip(values, min=-reach, max=reach).astype(kind)


def setup_inputs(seed: int = 0) -> dict:
    keys = jax.random.split(jax.random.key(seed), 8)
    hidden = normal_values(keys[0], (BATCH, TOKENS, D), 0.016, 0.09375, ((1, 8),))
    value_weight = normal_values(keys[1], (D, HEADS * DV), (D // 16) ** -0.5, 0.75, ((1, 4),))
    queries = normal_values(keys[2], (BATCH, HEADS, TOKENS, DK), 0.03, 0.1875, ((1, 4), (2, 8)))
    key_vectors = normal_values(keys[3], (BATCH, HEADS, TOKENS, DK), 0.03, 0.1875, ((1, 4), (2, 8)))
    forward_decay = jnp.clip(-0.005859375 + 0.005839844 * jax.random.uniform(keys[4], (BATCH, HEADS, TOKENS, DK), jnp.float32) ** steps_of(keys[4], (BATCH, HEADS, TOKENS, DK), ((1, 4), (2, 8)), -0.2, 0.2), -0.005859375, -1.9531249563442543e-05)
    backward_decay = jnp.clip(-0.005859375 + 0.005839844 * jax.random.uniform(keys[5], (BATCH, HEADS, TOKENS, DK), jnp.float32) ** steps_of(keys[5], (BATCH, HEADS, TOKENS, DK), ((1, 4), (2, 8)), -0.2, 0.2), -0.005859375, -1.9531249563442543e-05)
    cotangent = normal_values(keys[6], (BATCH, TOKENS, HEADS * DV), 1.0, 6.0, ((1, 8), (2, 4)))
    return dict(hidden=hidden, value_weight=value_weight, queries=queries, key_vectors=key_vectors, forward_decay=forward_decay, backward_decay=backward_decay, cotangent=cotangent)


EXACT_DOTS = lax.Precision.HIGHEST


def rounded(tensor):
    return lax.optimization_barrier(tensor.astype(jnp.bfloat16)).astype(jnp.float32)


def elements(query_heads, key_heads, value_heads, decay_heads, seed_heads):
    cumulative = jnp.cumsum(decay_heads, axis=2)
    final_sum = cumulative[:, :, -1, :]
    to_end = jnp.exp(final_sum[:, :, None, :] - cumulative)
    factor = jnp.exp(final_sum)
    state_part = jnp.einsum('bhjd,bhje->bhde', key_heads * to_end, value_heads, precision=EXACT_DOTS)
    grad_part = jnp.einsum('bhcd,bhce->bhde', query_heads * jnp.exp(cumulative), seed_heads, precision=EXACT_DOTS)
    return factor, state_part, grad_part


def block_grads(query_part, key_part, value_part, decay_part, seed_part, state_in, grad_in):
    length = query_part.shape[1]
    value_real = value_part.astype(jnp.float32)
    seed_real = seed_part.astype(jnp.float32)
    cumulative = jnp.cumsum(decay_part, axis=1)
    final_sum = cumulative[:, -1, :]
    growth = jnp.exp(cumulative)
    shrink = jnp.exp(-cumulative)
    to_end = jnp.exp(final_sum[:, None, :] - cumulative)
    query_hat = rounded(query_part * growth)
    key_hat = rounded(key_part * shrink)
    below_mask = jnp.tril(jnp.ones((length, length), dtype=bool))[None]
    scores = rounded(jnp.where(below_mask, jnp.einsum('hid,hjd->hij', query_hat, key_hat, precision=EXACT_DOTS), 0.0))
    seed_scores = rounded(jnp.where(below_mask, jnp.einsum('hie,hje->hij', seed_real, value_real, precision=EXACT_DOTS), 0.0))
    grad_query = growth * (jnp.einsum('hij,hjd->hid', seed_scores, key_hat, precision=EXACT_DOTS)
                           + jnp.einsum('hce,hde->hcd', seed_real, state_in, precision=EXACT_DOTS))
    grad_key = shrink * jnp.einsum('hij,hid->hjd', seed_scores, query_hat, precision=EXACT_DOTS)
    grad_key = grad_key + to_end * jnp.einsum('hde,hje->hjd', grad_in, value_real, precision=EXACT_DOTS)
    grad_value = jnp.einsum('hij,hie->hje', scores, seed_real, precision=EXACT_DOTS)
    grad_value = grad_value + jnp.einsum('hjd,hde->hje', key_part * to_end, grad_in, precision=EXACT_DOTS)
    grad_cumul = query_part * grad_query - key_part * grad_key
    return grad_query, grad_key, grad_value, grad_cumul


def direction(query_seq, key_seq, value_seq, decay_seq, seed_seq):
    head_count, length, key_width = query_seq.shape
    value_width = value_seq.shape[2]
    block_count = length // TOK_DEV

    def to_blocks(tensor):
        return tensor.reshape(head_count, block_count, TOK_DEV, tensor.shape[2]).transpose(1, 0, 2, 3)

    def from_blocks(tensor):
        return tensor.transpose(1, 0, 2, 3).reshape(head_count, length, tensor.shape[3])

    query_blocks, key_blocks = to_blocks(query_seq), to_blocks(key_seq)
    value_blocks, decay_blocks, seed_blocks = to_blocks(value_seq), to_blocks(decay_seq), to_blocks(seed_seq)
    factor, state_part, grad_part = elements(query_blocks, key_blocks, value_blocks.astype(jnp.float32),
                                             decay_blocks, seed_blocks.astype(jnp.float32))

    def advance(carried, pieces):
        return pieces[0][:, :, None] * carried + pieces[1], carried

    zero_state = jnp.zeros((head_count, key_width, value_width), jnp.float32)
    _, state_in = lax.scan(advance, zero_state, (factor, state_part))
    _, grad_in = lax.scan(advance, zero_state, (factor, grad_part), reverse=True)
    results = lax.map(lambda pieces: block_grads(*pieces),
                      (query_blocks, key_blocks, value_blocks, decay_blocks, seed_blocks, state_in, grad_in))
    return tuple(from_blocks(result) for result in results)


def reverse_tokens(tensor):
    return jnp.flip(tensor, axis=1)


def reference(hidden, value_weight, queries, key_vectors, forward_decay, backward_decay, cotangent):
    hidden_rows = hidden.reshape(BATCH * TOKENS, D)
    values_flat = jnp.dot(hidden_rows, value_weight, preferred_element_type=jnp.float32).astype(jnp.bfloat16)
    value_heads = values_flat.reshape(BATCH, TOKENS, HEADS, DV).transpose(0, 2, 1, 3)
    seed_heads = cotangent.reshape(BATCH, TOKENS, HEADS, DV).transpose(0, 2, 1, 3)

    def per_sequence(inputs):
        query_seq, key_seq, value_seq, ahead_decay, behind_decay, seed_seq = inputs
        ahead = direction(query_seq, key_seq, value_seq, ahead_decay, seed_seq)
        behind = direction(reverse_tokens(query_seq), reverse_tokens(key_seq), reverse_tokens(value_seq),
                           reverse_tokens(behind_decay), reverse_tokens(seed_seq))
        cumul_ahead = ahead[3]
        cumul_behind = reverse_tokens(behind[3])
        grad_ahead = -(jnp.cumsum(cumul_ahead, axis=1) - cumul_ahead)
        grad_behind = jnp.cumsum(cumul_behind, axis=1)
        return (ahead[0] + reverse_tokens(behind[0]), ahead[1] + reverse_tokens(behind[1]),
                ahead[2] + reverse_tokens(behind[2]), grad_ahead, grad_behind)

    grad_query, grad_key, grad_value, grad_ahead, grad_behind = lax.map(
        per_sequence, (queries.astype(jnp.float32), key_vectors.astype(jnp.float32), value_heads,
                       forward_decay, backward_decay, seed_heads))
    value_rows = grad_value.transpose(0, 2, 1, 3).reshape(BATCH * TOKENS, HEADS * DV).astype(jnp.bfloat16)
    grad_hidden = lax.dot_general(value_rows, value_weight, (((1,), (1,)), ((), ())),
                                  preferred_element_type=jnp.float32).astype(jnp.bfloat16).reshape(BATCH, TOKENS, D)
    grad_weight = lax.dot_general(hidden_rows, value_rows, (((0,), (0,)), ((), ())),
                                  preferred_element_type=jnp.float32)
    return (grad_query.astype(jnp.bfloat16), grad_key.astype(jnp.bfloat16), grad_ahead, grad_behind,
            grad_hidden, grad_weight)
```

```python
import functools

import jax
import jax.numpy as jnp
from jax import lax
from jax.experimental import pallas as pl
from jax.experimental.pallas import tpu as pltpu
from jax.sharding import PartitionSpec as P

F32, BF16 = jnp.float32, jnp.bfloat16
MESH = pl.DeviceIdType.MESH
LAG = 1


def dot(a, b, ca=1, cb=0):
    return lax.dot_general(a, b, (((ca,), (cb,)), ((), ())), preferred_element_type=F32)


def split(x):
    high = x.astype(BF16)
    return high, (x - high.astype(F32)).astype(BF16)


def plan(sp, batch, heads):
    outer = 4 if sp % 4 == 0 and batch % (sp // 4) == 0 else sp
    inner = sp // outer
    own = batch // inner
    return outer, inner, own, own * heads


def kernel(dims, hid, wgt, qry, key, fdec, bdec, cot,
           o_q, o_k, o_f, o_b, o_h, o_w,
           val, cum, intra_q, intra_k, intra_v,
           a_out, a_in, b_out, b_in, c_out, c_in, d_all, w_in, g_out, g_in,
           a_ss, a_rs, b_ss, b_rs, c_ss, c_rs, d_ss, d_rs, w_ss, w_rs, g_ss, g_rs):
    sp, tp, batch, heads, length, dk, dv, width = dims
    outer, inner, own, units = plan(sp, batch, heads)
    pack = 2 * dk
    feat = width // tp
    rows_sp = width // sp
    group = d_group(own)
    spi, tpi = lax.axis_index("sp"), lax.axis_index("tp")
    z, y = spi // inner, lax.rem(spi, inner)

    barrier = pltpu.get_barrier_semaphore()
    for r in range(1, sp):
        pl.semaphore_signal(barrier, inc=1, device_id={"sp": lax.rem(spi + r, sp)}, device_id_type=MESH)
    for r in range(1, tp):
        pl.semaphore_signal(barrier, inc=1, device_id={"tp": lax.rem(tpi + r, tp)}, device_id_type=MESH)
    pl.semaphore_wait(barrier, sp + tp - 2)

    def remote(src, dst, ss, rs, **where):
        return pltpu.make_async_remote_copy(src_ref=src, dst_ref=dst, send_sem=ss, recv_sem=rs,
                                            device_id=where, device_id_type=MESH)

    def w_copy(r):
        to = lax.rem(tpi + r, tp)
        return remote(wgt.at[pl.ds(pl.multiple_of(to * feat, feat), feat), :], w_in.at[r],
                      w_ss.at[r - 1], w_rs.at[r - 1], tp=to)

    def member(r):
        return lax.rem(y + r, inner)

    def a_copy(side, r, u):
        return remote(a_out.at[side, r - 1, u], a_in.at[side, r, u], a_ss.at[side, r - 1, u],
                      a_rs.at[side, r - 1, u], sp=z * inner + member(r))

    def b_copy(side, u):
        to = z + 1 if side == 0 else z - 1
        to = jnp.clip(to, 0, outer - 1)
        return remote(b_out.at[side, u], b_in.at[side, u], b_ss.at[side, u], b_rs.at[side, u],
                      sp=to * inner + y)

    def c_copy(side, r, u):
        return remote(c_out.at[side, r, u], c_in.at[side, r, u], c_ss.at[side, r - 1, u],
                      c_rs.at[side, r - 1, u], sp=z * inner + member(r))

    messages = own // group

    def d_copy(t, r, h, m):
        owner = lax.rem(y - r + inner, inner)
        first = pl.multiple_of((owner * own + m * group) * length, length)
        return remote(d_all.at[0, h, pl.ds(first, group * length), :],
                      d_all.at[t, h, pl.ds(first, group * length), :],
                      d_ss.at[t - 1, r, h, m], d_rs.at[t - 1, r, h, m], tp=lax.rem(tpi + t, tp))

    def d_wait(t, r, h, m):
        d_copy(t, r, h, m).wait_recv()

    def g_copy(r, h):
        to = lax.rem(spi + r, sp)
        return remote(g_out.at[h, to], g_in.at[h, r], g_ss.at[h, r - 1], g_rs.at[h, r - 1], sp=to)

    for r in range(1, tp):
        w_copy(r).start()
    w_in[0] = wgt[pl.ds(pl.multiple_of(tpi * feat, feat), feat), :]

    chunk = 4 * length
    total = batch * length

    def values(i, _):
        at = pl.ds(pl.multiple_of(i * chunk, chunk), chunk)
        val[at, :] = dot(hid[at, :], wgt[...]).astype(BF16)
        return 0

    lax.fori_loop(0, total // chunk, values, 0)

    row = lax.broadcasted_iota(jnp.int32, (length, length), 0)
    col = lax.broadcasted_iota(jnp.int32, (length, length), 1)
    lower, upper = row >= col, row <= col
    ones_lower, ones_upper = jnp.where(lower, 1.0, 0.0), jnp.where(upper, 1.0, 0.0)
    sums = jnp.concatenate([ones_lower, ones_upper], 0).astype(BF16)
    strict = jnp.concatenate([jnp.where(row > col, 1.0, 0.0), jnp.where(row < col, 1.0, 0.0)], 0).astype(BF16)
    left = lax.broadcasted_iota(jnp.int32, (length, pack), 1) < dk
    tail_row = lax.broadcasted_iota(jnp.int32, (16, pack), 0)
    ones_tail = jnp.ones((16, dv), BF16)
    ones_dv = jnp.ones((16, dv), BF16)

    def both(matrix, x):
        high, low = split(x)
        out = dot(matrix, high) + dot(matrix, low)
        return jnp.where(left, out[:length], out[length:])

    def head_cols(ref, b, h):
        at = pl.ds(pl.multiple_of(b * length, length), length)
        return ref[at, pl.ds(pl.multiple_of(h * dv, dv), dv)]

    def twice(ref, b, h):
        x = ref[b, h].astype(F32)
        return jnp.concatenate([x, x], 1)

    def parts(b, h):
        c = both(sums, jnp.concatenate([fdec[b, h], bdec[b, h]], 1))
        cum[b, h] = c
        end = jnp.where(left[:1], c[length - 1:length], c[0:1])
        grow = (twice(qry, b, h) * jnp.exp(c)).astype(BF16)
        decay_key = (twice(key, b, h) * jnp.exp(end - c)).astype(BF16)
        state = dot(decay_key, head_cols(val, b, h), 0, 0)
        grad = dot(grow, head_cols(cot, b, h), 0, 0)
        high = end.astype(BF16).astype(F32)
        tail = jnp.where(tail_row == 0, high, jnp.where(tail_row == 1, end - high, 0.0))
        low = jnp.concatenate([state[:dk], grad[dk:], tail], 0).astype(BF16)
        up = jnp.concatenate([grad[:dk], state[dk:], tail], 0).astype(BF16)
        return low, up

    def phase_one(u, _):
        h, step = u // own, lax.rem(u, own)
        made = [parts(member(r) * own + step, h) for r in range(inner)]
        for r in range(1, inner):
            for side in range(2):
                a_out[side, r - 1, u] = made[r][side]
        for side in range(2):
            a_in[side, 0, u] = made[0][side]
        for r in range(1, inner):
            for side in range(2):
                a_copy(side, r, u).start()
        return 0

    lax.fori_loop(0, units, phase_one, 0)

    def intra(b, h):
        c = cum[b, h]
        q_hat = (twice(qry, b, h) * jnp.exp(c)).astype(BF16)
        k_hat = (twice(key, b, h) * jnp.exp(-c)).astype(BF16)
        v, seed = head_cols(val, b, h), head_cols(cot, b, h)
        seed_scores = dot(seed, v, 1, 1)
        zero = jnp.zeros_like(q_hat)
        q_left, q_right = jnp.where(left, q_hat, zero), jnp.where(left, zero, q_hat)
        k_left, k_right = jnp.where(left, k_hat, zero), jnp.where(left, zero, k_hat)
        score = (jnp.where(lower, dot(q_left, k_hat, 1, 1), 0.0)
                 + jnp.where(upper, dot(q_right, k_hat, 1, 1), 0.0)).astype(BF16)
        seed_low = jnp.where(lower, seed_scores, 0.0).astype(BF16)
        seed_up = jnp.where(upper, seed_scores, 0.0).astype(BF16)
        intra_q[b, h] = dot(seed_low, k_left) + dot(seed_up, k_right)
        intra_k[b, h] = dot(seed_low, q_left, 0, 0) + dot(seed_up, q_right, 0, 0)
        intra_v[b, h] = dot(score, seed, 0, 0)

    def combine(side, u):
        @pl.when((z > 0) if side == 0 else (z < outer - 1))
        def _():
            b_copy(side, u).wait_recv()

        first = (z == 0) if side == 0 else (z == outer - 1)

        @pl.when(first)
        def _():
            b_in[side, u] = jnp.zeros((pack, dv), BF16)

        for r in range(1, inner):
            a_copy(side, r, u).wait_recv()
        running = b_in[side, u].astype(F32)
        order = range(inner) if side == 0 else range(inner - 1, -1, -1)
        for person in order:
            r = lax.rem(person - y + inner, inner)
            source = lax.rem(y - person + inner, inner)
            c_out[side, r, u] = running.astype(BF16)
            message = a_in[side, source, u]
            factor = jnp.exp(dot(message[pack:], ones_tail, 0, 0))
            running = factor * running + message[:pack].astype(F32)
        b_out[side, u] = running.astype(BF16)

        @pl.when((z < outer - 1) if side == 0 else (z > 0))
        def _():
            b_copy(side, u).start()

        c_in[side, 0, u] = c_out[side, 0, u]
        for r in range(1, inner):
            c_copy(side, r, u).start()

    def finish(r, u, h, step):
        b = lax.rem(y - r + inner, inner) * own + step
        low, up = c_in[0, r, u], c_in[1, r, u]
        state = jnp.concatenate([low[:dk], up[dk:]], 0)
        grad = jnp.concatenate([up[:dk], low[dk:]], 0)
        c = cum[b, h]
        end = jnp.where(left[:1], c[length - 1:length], c[0:1])
        grow, shrink, to_end = jnp.exp(c), jnp.exp(-c), jnp.exp(end - c)
        q, k = twice(qry, b, h), twice(key, b, h)
        v, seed = head_cols(val, b, h), head_cols(cot, b, h)
        cross = dot(seed, state, 1, 1)
        dq = grow * (intra_q[b, h] + cross)
        dk_ = shrink * intra_k[b, h] + to_end * dot(v, grad, 1, 1)
        dv_ = intra_v[b, h] + dot((k * to_end).astype(BF16), grad)
        g = q * dq - k * dk_
        pair = (state.astype(F32) * grad.astype(F32)).astype(BF16)
        start = (jnp.sum(q * grow * cross, axis=0, keepdims=True)
                 + jnp.exp(end) * dot(ones_dv, pair, 1, 1)[:1])
        decay_grad = start - both(strict, g)
        o_q[b, h] = (dq[:, :dk] + dq[:, dk:]).astype(BF16)
        o_k[b, h] = (dk_[:, :dk] + dk_[:, dk:]).astype(BF16)
        o_f[b, h] = decay_grad[:, :dk]
        o_b[b, h] = decay_grad[:, dk:]
        d_all[0, h, pl.ds(pl.multiple_of(b * length, length), length), :] = dv_.astype(BF16)

    def weight_term(h):
        full = dot(d_all[0, h], hid[...], 0, 0)
        for p in range(sp):
            g_out[h, p] = full[:, p * rows_sp:(p + 1) * rows_sp].astype(BF16)
        for r in range(1, sp):
            g_copy(r, h).start()

    reach = (outer - 1) * LAG
    delay = reach + 1

    def phase_two(s, _):
        @pl.when(s < units)
        def _():
            h, step = s // own, lax.rem(s, own)
            for r in range(inner):
                intra(r * own + step, h)

        for side in range(2):
            at = s - (z if side == 0 else outer - 1 - z) * LAG

            @pl.when((at >= 0) & (at < units))
            def _():
                combine(side, at)

        last = s - delay

        @pl.when(last >= 0)
        def _():
            h, step = last // own, lax.rem(last, own)
            for side in range(2):
                for r in range(1, inner):
                    c_copy(side, r, last).wait_recv()
            for r in range(inner):
                finish(r, last, h, step)

            @pl.when(lax.rem(step + 1, group) == 0)
            def _():
                m = step // group
                for r in range(inner):
                    for t in range(1, tp):
                        d_copy(t, r, h, m).start()

            @pl.when(step == own - 1)
            def _():
                weight_term(h)
        return 0

    lax.fori_loop(0, units + delay, phase_two, 0)

    for t in range(1, tp):
        w_copy(t).wait_recv()
        for r in range(inner):
            for h in range(heads):
                for m in range(messages):
                    d_wait(t, r, h, m)

    def features(i, _):
        at = pl.ds(pl.multiple_of(i * chunk, chunk), chunk)
        acc = jnp.zeros((chunk, feat), F32)
        for t in range(tp):
            for h in range(heads):
                acc = acc + dot(d_all[t, h, at, :], w_in[t, :, h * dv:(h + 1) * dv], 1, 1)
        o_h[at, :] = acc.astype(BF16)
        return 0

    lax.fori_loop(0, total // chunk, features, 0)

    for h in range(heads):
        acc = g_out[h, spi].astype(F32)
        for r in range(1, sp):
            g_copy(r, h).wait_recv()
            acc = acc + g_in[h, r].astype(F32)
        o_w[:, h * dv:(h + 1) * dv] = acc.T

    for r in range(1, tp):
        w_copy(r).wait_send()
    for h in range(heads):
        for r in range(1, sp):
            g_copy(r, h).wait_send()
        for m in range(messages):
            for t in range(1, tp):
                for r in range(inner):
                    d_copy(t, r, h, m).wait_send()

    def drain(u, _):
        for side in range(2):
            for r in range(1, inner):
                a_copy(side, r, u).wait_send()
                c_copy(side, r, u).wait_send()

            @pl.when((z < outer - 1) if side == 0 else (z > 0))
            def _():
                b_copy(side, u).wait_send()
        return 0

    lax.fori_loop(0, units, drain, 0)


def d_group(own):
    return 4 if own % 4 == 0 else 1


def shards(sp, tp, hidden, value_weight, queries, key_vectors, forward_decay, backward_decay, cotangent):
    batch, length, width = hidden.shape
    heads, dk = queries.shape[1], queries.shape[3]
    cols = value_weight.shape[1]
    dv = cols // heads
    outer, inner, own, units = plan(sp, batch, heads)
    pack, rows, feat, rows_sp = 2 * dk, batch * length, width // tp, width // sp
    group = d_group(own)
    dims = (sp, tp, batch, heads, length, dk, dv, width)
    vmem, dma = pltpu.VMEM, pltpu.SemaphoreType.DMA
    peers = max(inner - 1, 1)
    scratch = [
        vmem((rows, cols), BF16),
        vmem((batch, heads, length, pack), F32),
        vmem((batch, heads, length, pack), F32),
        vmem((batch, heads, length, pack), F32),
        vmem((batch, heads, length, dv), F32),
        vmem((2, peers, units, pack + 16, dv), BF16),
        vmem((2, inner, units, pack + 16, dv), BF16),
        vmem((2, units, pack, dv), BF16),
        vmem((2, units, pack, dv), BF16),
        vmem((2, inner, units, pack, dv), BF16),
        vmem((2, inner, units, pack, dv), BF16),
        vmem((tp, heads, rows, dv), BF16),
        vmem((tp, feat, cols), BF16),
        vmem((heads, sp, dv, rows_sp), BF16),
        vmem((heads, sp, dv, rows_sp), BF16),
        dma((2, peers, units)), dma((2, peers, units)),
        dma((2, units)), dma((2, units)),
        dma((2, peers, units)), dma((2, peers, units)),
        dma((tp - 1, inner, heads, own // group)), dma((tp - 1, inner, heads, own // group)),
        dma((tp - 1,)), dma((tp - 1,)),
        dma((heads, sp - 1)), dma((heads, sp - 1)),
    ]
    whole = pl.BlockSpec(memory_space=vmem)
    outs = pl.pallas_call(
        functools.partial(kernel, dims),
        out_shape=(
            jax.ShapeDtypeStruct(queries.shape, BF16),
            jax.ShapeDtypeStruct(queries.shape, BF16),
            jax.ShapeDtypeStruct(queries.shape, F32),
            jax.ShapeDtypeStruct(queries.shape, F32),
            jax.ShapeDtypeStruct((rows, feat), BF16),
            jax.ShapeDtypeStruct((rows_sp, cols), F32),
        ),
        in_specs=[whole] * 7,
        out_specs=(whole,) * 6,
        scratch_shapes=scratch,
        compiler_params=pltpu.CompilerParams(
            collective_id=0, has_side_effects=True, vmem_limit_bytes=60 * 1024 * 1024
        ),
    )(hidden.reshape(rows, width), value_weight, queries, key_vectors, forward_decay, backward_decay,
      cotangent.reshape(rows, cols))
    return (outs[0], outs[1], outs[2], outs[3], outs[4].reshape(batch, length, feat), outs[5])


def solution(mesh):
    heads = P(None, "tp", "sp", None)
    return jax.shard_map(
        functools.partial(shards, mesh.shape["sp"], mesh.shape["tp"]),
        mesh=mesh,
        in_specs=(P(None, "sp", None), P(None, "tp"), heads, heads, heads, heads, P(None, "sp", "tp")),
        out_specs=(heads, heads, heads, heads, P(None, "sp", "tp"), P("sp", "tp")),
        check_vma=False,
    )
```

```python
import functools

import jax
import jax.numpy as jnp
from jax import lax
from jax.experimental import pallas as pl
from jax.experimental.pallas import tpu as pltpu
from jax.sharding import PartitionSpec as P

F32, BF16 = jnp.float32, jnp.bfloat16
MESH = pl.DeviceIdType.MESH
LAG = 2
EXTRA = 4


def dot(a, b, ca=1, cb=0):
    return lax.dot_general(a, b, (((ca,), (cb,)), ((), ())), preferred_element_type=F32)


def split(x):
    high = x.astype(BF16)
    return high, (x - high.astype(F32)).astype(BF16)


def plan(sp, batch, heads):
    outer = 4 if sp % 4 == 0 and batch % (sp // 4) == 0 else sp
    inner = sp // outer
    own = batch // inner
    return outer, inner, own, own * heads


def kernel(dims, hid, wgt, qry, key, fdec, bdec, cot,
           o_qk, o_fb, o_h, o_w,
           val, cum, intra_q, intra_k, intra_v,
           a_out, a_in, b_out, b_in, c_out, c_in, d_all, w_in, g_out, g_in,
           a_ss, a_rs, b_ss, b_rs, c_ss, c_rs, d_ss, d_rs, w_ss, w_rs, g_ss, g_rs):
    sp, tp, batch, heads, length, dk, dv, width = dims
    outer, inner, own, units = plan(sp, batch, heads)
    pack = 2 * dk
    feat = width // tp
    rows_sp = width // sp
    group = d_group(own)
    spi, tpi = lax.axis_index("sp"), lax.axis_index("tp")
    z, y = spi // inner, lax.rem(spi, inner)

    barrier = pltpu.get_barrier_semaphore()
    for r in range(1, sp):
        pl.semaphore_signal(barrier, inc=1, device_id={"sp": lax.rem(spi + r, sp)}, device_id_type=MESH)
    for r in range(1, tp):
        pl.semaphore_signal(barrier, inc=1, device_id={"tp": lax.rem(tpi + r, tp)}, device_id_type=MESH)
    pl.semaphore_wait(barrier, sp + tp - 2)

    def remote(src, dst, ss, rs, **where):
        return pltpu.make_async_remote_copy(src_ref=src, dst_ref=dst, send_sem=ss, recv_sem=rs,
                                            device_id=where, device_id_type=MESH)

    def w_copy(r):
        to = lax.rem(tpi + r, tp)
        return remote(wgt.at[pl.ds(pl.multiple_of(to * feat, feat), feat), :], w_in.at[r],
                      w_ss.at[r - 1], w_rs.at[r - 1], tp=to)

    def member(r):
        return lax.rem(y + r, inner)

    def a_copy(side, r, u):
        return remote(a_out.at[side, r - 1, u], a_in.at[side, r, u], a_ss.at[side, r - 1, u],
                      a_rs.at[side, r - 1, u], sp=z * inner + member(r))

    def b_copy(side, u):
        to = z + 1 if side == 0 else z - 1
        to = jnp.clip(to, 0, outer - 1)
        return remote(b_out.at[side, u], b_in.at[side, u], b_ss.at[side, u], b_rs.at[side, u],
                      sp=to * inner + y)

    def c_copy(side, r, u):
        return remote(c_out.at[side, r, u], c_in.at[side, r, u], c_ss.at[side, r - 1, u],
                      c_rs.at[side, r - 1, u], sp=z * inner + member(r))

    messages = own // group

    def d_copy(t, r, h, m):
        owner = lax.rem(y - r + inner, inner)
        first = pl.multiple_of((owner * own + m * group) * length, length)
        return remote(d_all.at[0, h, pl.ds(first, group * length), :],
                      d_all.at[t, h, pl.ds(first, group * length), :],
                      d_ss.at[t - 1, r, h, m], d_rs.at[t - 1, r, h, m], tp=lax.rem(tpi + t, tp))

    def d_wait(t, r, h, m):
        d_copy(t, r, h, m).wait_recv()

    def g_copy(r, h):
        to = lax.rem(spi + r, sp)
        return remote(g_out.at[h, to], g_in.at[h, r], g_ss.at[h, r - 1], g_rs.at[h, r - 1], sp=to)

    for r in range(1, tp):
        w_copy(r).start()
    w_in[0] = wgt[pl.ds(pl.multiple_of(tpi * feat, feat), feat), :]

    chunk = 4 * length
    total = batch * length

    def values(i, _):
        at = pl.ds(pl.multiple_of(i * chunk, chunk), chunk)
        val[at, :] = dot(hid[at, :], wgt[...]).astype(BF16)
        return 0

    mine = own * length // chunk if own * length % chunk == 0 else 0

    def values_of(r):
        lax.fori_loop(0, mine, lambda i, _: values(member(r) * mine + i, 0), 0)

    if mine:
        for r in range(1, inner):
            values_of(r)
    else:
        lax.fori_loop(0, total // chunk, values, 0)

    row = lax.broadcasted_iota(jnp.int32, (length, length), 0)
    col = lax.broadcasted_iota(jnp.int32, (length, length), 1)
    lower, upper = row >= col, row <= col
    ones_lower, ones_upper = jnp.where(lower, 1.0, 0.0), jnp.where(upper, 1.0, 0.0)
    sums = jnp.concatenate([ones_lower, ones_upper], 0).astype(BF16)
    strict = jnp.concatenate([jnp.where(row > col, 1.0, 0.0), jnp.where(row < col, 1.0, 0.0)], 0).astype(BF16)
    left = lax.broadcasted_iota(jnp.int32, (length, pack), 1) < dk
    tail_row = lax.broadcasted_iota(jnp.int32, (16, pack), 0)
    ones_tail = jnp.ones((16, dv), BF16)
    ones_dv = jnp.ones((16, dv), BF16)

    def both(matrix, x):
        high, low = split(x)
        out = dot(matrix, high) + dot(matrix, low)
        return jnp.where(left, out[:length], out[length:])

    def head_cols(ref, b, h):
        at = pl.ds(pl.multiple_of(b * length, length), length)
        return ref[at, pl.ds(pl.multiple_of(h * dv, dv), dv)]

    def twice(ref, b, h):
        x = ref[b, h].astype(F32)
        return jnp.concatenate([x, x], 1)

    def parts(b, h):
        c = both(sums, jnp.concatenate([fdec[b, h], bdec[b, h]], 1))
        cum[b, h] = c
        end = jnp.where(left[:1], c[length - 1:length], c[0:1])
        grow = (twice(qry, b, h) * jnp.exp(c)).astype(BF16)
        decay_key = (twice(key, b, h) * jnp.exp(end - c)).astype(BF16)
        state = dot(decay_key, head_cols(val, b, h), 0, 0)
        grad = dot(grow, head_cols(cot, b, h), 0, 0)
        high = end.astype(BF16).astype(F32)
        tail = jnp.where(tail_row == 0, high, jnp.where(tail_row == 1, end - high, 0.0))
        low = jnp.concatenate([state[:dk], grad[dk:], tail], 0).astype(BF16)
        up = jnp.concatenate([grad[:dk], state[dk:], tail], 0).astype(BF16)
        return low, up

    pair = 2 if units % 2 == 0 else 1

    def phase_one(i, _):
        todo = [(r, i * pair + n) for n in range(pair) for r in range(1, inner)]
        made = [parts(member(r) * own + lax.rem(u, own), u // own) for r, u in todo]
        for (r, u), sides in zip(todo, made):
            for side in range(2):
                a_out[side, r - 1, u] = sides[side]
        for r, u in todo:
            for side in range(2):
                a_copy(side, r, u).start()
        return 0

    lax.fori_loop(0, units // pair, phase_one, 0)
    if mine:
        values_of(0)

    def intra(b, h):
        c = cum[b, h]
        q_hat = (twice(qry, b, h) * jnp.exp(c)).astype(BF16)
        k_hat = (twice(key, b, h) * jnp.exp(-c)).astype(BF16)
        v, seed = head_cols(val, b, h), head_cols(cot, b, h)
        seed_scores = dot(seed, v, 1, 1)
        zero = jnp.zeros_like(q_hat)
        q_left, q_right = jnp.where(left, q_hat, zero), jnp.where(left, zero, q_hat)
        k_left, k_right = jnp.where(left, k_hat, zero), jnp.where(left, zero, k_hat)
        score = (jnp.where(lower, dot(q_left, k_hat, 1, 1), 0.0)
                 + jnp.where(upper, dot(q_right, k_hat, 1, 1), 0.0)).astype(BF16)
        seed_low = jnp.where(lower, seed_scores, 0.0).astype(BF16)
        seed_up = jnp.where(upper, seed_scores, 0.0).astype(BF16)
        intra_q[b, h] = dot(seed_low, k_left) + dot(seed_up, k_right)
        intra_k[b, h] = dot(seed_low, q_left, 0, 0) + dot(seed_up, q_right, 0, 0)
        intra_v[b, h] = dot(score, seed, 0, 0)

    def combine(side, u):
        @pl.when((z > 0) if side == 0 else (z < outer - 1))
        def _():
            b_copy(side, u).wait_recv()

        first = (z == 0) if side == 0 else (z == outer - 1)

        @pl.when(first)
        def _():
            b_in[side, u] = jnp.zeros((pack, dv), BF16)

        for r in range(1, inner):
            a_copy(side, r, u).wait_recv()
        running = b_in[side, u].astype(F32)
        order = range(inner) if side == 0 else range(inner - 1, -1, -1)
        for person in order:
            r = lax.rem(person - y + inner, inner)
            source = lax.rem(y - person + inner, inner)
            c_out[side, r, u] = running.astype(BF16)
            message = a_in[side, source, u]
            factor = jnp.exp(dot(message[pack:], ones_tail, 0, 0))
            running = factor * running + message[:pack].astype(F32)
        b_out[side, u] = running.astype(BF16)

        @pl.when((z < outer - 1) if side == 0 else (z > 0))
        def _():
            b_copy(side, u).start()

        c_in[side, 0, u] = c_out[side, 0, u]
        for r in range(1, inner):
            c_copy(side, r, u).start()

    def finish(r, u, h, step):
        b = lax.rem(y - r + inner, inner) * own + step
        low, up = c_in[0, r, u], c_in[1, r, u]
        state = jnp.concatenate([low[:dk], up[dk:]], 0)
        grad = jnp.concatenate([up[:dk], low[dk:]], 0)
        c = cum[b, h]
        end = jnp.where(left[:1], c[length - 1:length], c[0:1])
        grow, shrink, to_end = jnp.exp(c), jnp.exp(-c), jnp.exp(end - c)
        q, k = twice(qry, b, h), twice(key, b, h)
        v, seed = head_cols(val, b, h), head_cols(cot, b, h)
        cross = dot(seed, state, 1, 1)
        dq = grow * (intra_q[b, h] + cross)
        dk_ = shrink * intra_k[b, h] + to_end * dot(v, grad, 1, 1)
        dv_ = intra_v[b, h] + dot((k * to_end).astype(BF16), grad)
        g = q * dq - k * dk_
        pair = (state.astype(F32) * grad.astype(F32)).astype(BF16)
        start = (jnp.sum(q * grow * cross, axis=0, keepdims=True)
                 + jnp.exp(end) * dot(ones_dv, pair, 1, 1)[:1])
        decay_grad = start - both(strict, g)
        o_qk[b, h] = jnp.concatenate([dq[:, :dk] + dq[:, dk:], dk_[:, :dk] + dk_[:, dk:]], 1).astype(BF16)
        o_fb[b, h] = decay_grad
        d_all[0, h, pl.ds(pl.multiple_of(b * length, length), length), :] = dv_.astype(BF16)

    def weight_term(h):
        full = dot(d_all[0, h], hid[...], 0, 0)
        for p in range(sp):
            g_out[h, p] = full[:, p * rows_sp:(p + 1) * rows_sp].astype(BF16)
        for r in range(1, sp):
            g_copy(r, h).start()

    delay = (outer - 1) * LAG + 1 + EXTRA

    def phase_two(s, _):
        for side in range(2):
            at = s - 1 - (z if side == 0 else outer - 1 - z) * LAG

            @pl.when((at >= 0) & (at < units))
            def _():
                combine(side, at)

        @pl.when(s < units)
        def _():
            h, step = s // own, lax.rem(s, own)
            low, up = parts(y * own + step, h)
            a_in[0, 0, s] = low
            a_in[1, 0, s] = up
            for r in range(inner):
                intra(member(r) * own + step, h)

        last = s - delay

        @pl.when(last >= 0)
        def _():
            h, step = last // own, lax.rem(last, own)
            for side in range(2):
                for r in range(1, inner):
                    c_copy(side, r, last).wait_recv()
            for r in range(inner):
                finish(r, last, h, step)

            @pl.when(lax.rem(step + 1, group) == 0)
            def _():
                m = step // group
                for r in range(inner):
                    for t in range(1, tp):
                        d_copy(t, r, h, m).start()

            @pl.when(step == own - 1)
            def _():
                weight_term(h)
        return 0

    lax.fori_loop(0, units + delay, phase_two, 0)

    for t in range(1, tp):
        w_copy(t).wait_recv()
        for r in range(inner):
            for h in range(heads):
                for m in range(messages):
                    d_wait(t, r, h, m)

    def features(i, _):
        at = pl.ds(pl.multiple_of(i * chunk, chunk), chunk)
        acc = jnp.zeros((chunk, feat), F32)
        for t in range(tp):
            for h in range(heads):
                acc = acc + dot(d_all[t, h, at, :], w_in[t, :, h * dv:(h + 1) * dv], 1, 1)
        o_h[at, :] = acc.astype(BF16)
        return 0

    lax.fori_loop(0, total // chunk, features, 0)

    for h in range(heads):
        acc = g_out[h, spi].astype(F32)
        for r in range(1, sp):
            g_copy(r, h).wait_recv()
            acc = acc + g_in[h, r].astype(F32)
        o_w[:, h * dv:(h + 1) * dv] = acc.T

    for r in range(1, tp):
        w_copy(r).wait_send()
    for h in range(heads):
        for r in range(1, sp):
            g_copy(r, h).wait_send()
        for m in range(messages):
            for t in range(1, tp):
                for r in range(inner):
                    d_copy(t, r, h, m).wait_send()

    def drain(u, _):
        for side in range(2):
            for r in range(1, inner):
                a_copy(side, r, u).wait_send()
                c_copy(side, r, u).wait_send()

            @pl.when((z < outer - 1) if side == 0 else (z > 0))
            def _():
                b_copy(side, u).wait_send()
        return 0

    lax.fori_loop(0, units, drain, 0)


def d_group(own):
    return 4 if own % 4 == 0 else 1


def shards(sp, tp, hidden, value_weight, queries, key_vectors, forward_decay, backward_decay, cotangent):
    batch, length, width = hidden.shape
    heads, dk = queries.shape[1], queries.shape[3]
    cols = value_weight.shape[1]
    dv = cols // heads
    outer, inner, own, units = plan(sp, batch, heads)
    pack, rows, feat, rows_sp = 2 * dk, batch * length, width // tp, width // sp
    group = d_group(own)
    dims = (sp, tp, batch, heads, length, dk, dv, width)
    vmem, dma = pltpu.VMEM, pltpu.SemaphoreType.DMA
    peers = max(inner - 1, 1)
    scratch = [
        vmem((rows, cols), BF16),
        vmem((batch, heads, length, pack), F32),
        vmem((batch, heads, length, pack), F32),
        vmem((batch, heads, length, pack), F32),
        vmem((batch, heads, length, dv), F32),
        vmem((2, peers, units, pack + 16, dv), BF16),
        vmem((2, inner, units, pack + 16, dv), BF16),
        vmem((2, units, pack, dv), BF16),
        vmem((2, units, pack, dv), BF16),
        vmem((2, inner, units, pack, dv), BF16),
        vmem((2, inner, units, pack, dv), BF16),
        vmem((tp, heads, rows, dv), BF16),
        vmem((tp, feat, cols), BF16),
        vmem((heads, sp, dv, rows_sp), BF16),
        vmem((heads, sp, dv, rows_sp), BF16),
        dma((2, peers, units)), dma((2, peers, units)),
        dma((2, units)), dma((2, units)),
        dma((2, peers, units)), dma((2, peers, units)),
        dma((tp - 1, inner, heads, own // group)), dma((tp - 1, inner, heads, own // group)),
        dma((tp - 1,)), dma((tp - 1,)),
        dma((heads, sp - 1)), dma((heads, sp - 1)),
    ]
    whole = pl.BlockSpec(memory_space=vmem)
    outs = pl.pallas_call(
        functools.partial(kernel, dims),
        out_shape=(
            jax.ShapeDtypeStruct((batch, heads, length, pack), BF16),
            jax.ShapeDtypeStruct((batch, heads, length, pack), F32),
            jax.ShapeDtypeStruct((rows, feat), BF16),
            jax.ShapeDtypeStruct((rows_sp, cols), F32),
        ),
        in_specs=[whole] * 7,
        out_specs=(whole,) * 4,
        scratch_shapes=scratch,
        compiler_params=pltpu.CompilerParams(
            collective_id=0, has_side_effects=True, vmem_limit_bytes=60 * 1024 * 1024
        ),
    )(hidden.reshape(rows, width), value_weight, queries, key_vectors, forward_decay, backward_decay,
      cotangent.reshape(rows, cols))
    near, decays = outs[0], outs[1]
    return (near[..., :dk], near[..., dk:], decays[..., :dk], decays[..., dk:],
            outs[2].reshape(batch, length, feat), outs[3])


def solution(mesh):
    heads = P(None, "tp", "sp", None)
    return jax.shard_map(
        functools.partial(shards, mesh.shape["sp"], mesh.shape["tp"]),
        mesh=mesh,
        in_specs=(P(None, "sp", None), P(None, "tp"), heads, heads, heads, heads, P(None, "sp", "tp")),
        out_specs=(heads, heads, heads, heads, P(None, "sp", "tp"), P("sp", "tp")),
        check_vma=False,
    )
```
